128 devices in a mesh: sp: 32 (over z, y, core), tp: 4 (over x).
Axes of the slice: x: 4, y: 4, z: 4, core: 2. Of those that a mesh axis runs over, the one named last changes fastest.
Arguments:
- tokens: bfloat16 [8192, 1024], P(('sp', 'tp')), may hold values from -7.5 to 7.5, as said below
- query_weight: bfloat16 [1024, 2048], P('sp', 'tp'), may hold values from -0.1875 to 0.1875
- key_weight: bfloat16 [1024, 2048], P('sp', 'tp'), may hold values from -0.1875 to 0.1875
- value_weight: bfloat16 [1024, 2048], P('sp', 'tp'), may hold values from -0.1875 to 0.1875
- gate_weight: bfloat16 [1024, 16], P('sp', 'tp'), may hold values from -0.1875 to 0.1875
- forget_bias: float32 [16], P('tp'), may hold values from 0 to 2
- out_weight: bfloat16 [2048, 1024], P('tp', 'sp'), may hold values from -0.125 to 0.125
- out_gain: float32 [1024], replicated, may hold values from 0.5 to 1.5
Outputs:
- mixed: bfloat16 [8192, 1024], P(('sp', 'tp'))
The draws below stay inside these ranges and needn't reach their ends.
Inputs may be any that keep to these rules, and one draw needn't show every extreme that they name: `tokens`: each entry is a bounded noise value (at most 6 in size) plus an offset in -1.5 to 1.5 shared by the 256 rows of one index of sp, so every entry lies within -7.5 and 7.5.
All inputs are finite; a program needn't handle non-finite values.
Results may differ from the reference program's by a relative error of at most 0.006.
Values may be sent and summed in bfloat16 or wider, within the bound.
A program may use at most 128 MiB of HBM per device.

```python
import math
import jax
import jax.numpy as jnp
from jax import lax

D = 1024
HEADS = 16
HEAD_DIM = 128
TOK_DEV = 256
WIDTH = 2048
SEQ = 8192


def draw_tokens(key, part):
    noise_key = jax.random.fold_in(key, 11)
    shift_key = jax.random.fold_in(key, 12)
    noise = jax.random.truncated_normal(noise_key, -6.0, 6.0, (SEQ, D), jnp.float32)
    shifts = jax.random.uniform(shift_key, (SEQ // TOK_DEV, D), jnp.float32, -1.5, 1.5)
    return (noise + jnp.repeat(shifts, TOK_DEV, axis=0)).astype(jnp.bfloat16)


def block_scale(stream_key, extent, cuts, low, top_value):
    level = 1.0
    for dim, shards_of in cuts:
        draws = jax.random.uniform(jax.random.fold_in(jax.random.fold_in(stream_key, 6), dim), (shards_of,), jnp.float32, low / len(cuts), top_value / len(cuts))
        level = level * jnp.repeat(jnp.exp(draws), extent[dim] // shards_of).reshape((-1,) + (1,) * (len(extent) - 1 - dim))
    return level


def gaussian(own_key, dims, width, most, cuts=(), kind=jnp.bfloat16):
    factor_of = block_scale(own_key, dims, cuts, -0.22, 0.18) if cuts else 1.0
    values = jax.random.normal(own_key, dims, jnp.float32) * width * factor_of
    return jnp.minimum(jnp.maximum(values, -most), most).astype(kind)


def setup_inputs(seed: int = 0) -> dict:
    key_of = jax.random.split(jax.random.key(seed), 9)
    tokens = draw_tokens(jax.random.fold_in(key_of[8], 71), 0)
    query_weight = gaussian(key_of[1], (D, WIDTH), D ** -0.5, 0.1875, ((0, 32), (1, 4)))
    key_weight = gaussian(key_of[2], (D, WIDTH), D ** -0.5, 0.1875, ((0, 32), (1, 4)))
    value_weight = gaussian(key_of[3], (D, WIDTH), D ** -0.5, 0.1875, ((0, 32), (1, 4)))
    gate_weight = gaussian(key_of[4], (D, HEADS), D ** -0.5, 0.1875, ((0, 32), (1, 4)))
    forget_bias = jnp.clip(2.0 * jax.random.uniform(key_of[5], (HEADS,), jnp.float32) ** block_scale(key_of[5], (HEADS,), ((0, 4),), -0.2, 0.2), 0.0, 2.0)
    out_weight = gaussian(key_of[6], (WIDTH, D), WIDTH ** -0.5, 0.125, ((0, 4), (1, 32)))
    out_gain = jnp.clip(1.0 + 0.1 * jax.random.normal(key_of[7], (D,), jnp.float32), 0.5, 1.5)
    return {"tokens": tokens, "query_weight": query_weight, "key_weight": key_weight, "value_weight": value_weight, "gate_weight": gate_weight, "forget_bias": forget_bias, "out_weight": out_weight, "out_gain": out_gain}


def reference(tokens, query_weight, key_weight, value_weight, gate_weight, forget_bias, out_weight, out_gain):
    queries = jnp.dot(tokens, query_weight, preferred_element_type=jnp.float32).astype(jnp.bfloat16)
    keys = jnp.dot(tokens, key_weight, preferred_element_type=jnp.float32).astype(jnp.bfloat16)
    values = jnp.dot(tokens, value_weight, preferred_element_type=jnp.float32).astype(jnp.bfloat16)
    queries = queries.reshape(SEQ, HEADS, HEAD_DIM).astype(jnp.float32)
    keys = keys.reshape(SEQ, HEADS, HEAD_DIM).astype(jnp.float32)
    values = values.reshape(SEQ, HEADS, HEAD_DIM).astype(jnp.float32)
    raw_gate = jnp.dot(tokens, gate_weight, preferred_element_type=jnp.float32)
    log_gate = jax.nn.log_sigmoid(raw_gate + forget_bias + math.log(SEQ))
    cumulative = jnp.cumsum(log_gate, axis=0)
    scale = HEAD_DIM ** (-0.5)
    key_pos = jnp.arange(SEQ, dtype=jnp.int32)

    def one_block(index):
        start = (index * TOK_DEV).astype(jnp.int32)
        block_q = lax.dynamic_slice_in_dim(queries, start, TOK_DEV, 0)
        block_c = lax.dynamic_slice_in_dim(cumulative, start, TOK_DEV, 0)
        logits = jnp.einsum('qhd,khd->hqk', block_q, keys) * scale
        logits = logits + block_c.T[:, :, None] - cumulative.T[:, None, :]
        query_pos = start + jnp.arange(TOK_DEV, dtype=jnp.int32)
        allowed = key_pos[None, :] <= query_pos[:, None]
        logits = jnp.where(allowed[None], logits, -1e+30)
        weights = jax.nn.softmax(logits, axis=-1)
        result = jnp.einsum('hqk,khd->qhd', weights, values)
        return result.reshape(TOK_DEV, WIDTH).astype(jnp.bfloat16)
    attended = lax.map(one_block, jnp.arange(SEQ // TOK_DEV, dtype=jnp.int32)).reshape(SEQ, WIDTH)
    summed = jnp.dot(attended, out_weight, preferred_element_type=jnp.float32)
    normed = summed * lax.rsqrt(lax.optimization_barrier(jnp.mean(summed * summed, axis=-1, keepdims=True)) + 1e-06)
    return (normed * out_gain).astype(jnp.bfloat16)
```

```python
import math

import jax
import jax.numpy as jnp
from jax import lax
from jax.experimental import pallas as pl
from jax.experimental.pallas import tpu as pltpu
from jax.sharding import Mesh
from jax.sharding import PartitionSpec as P

SP = ("z", "y", "c")
SP_TP = ("z", "y", "c", "x")
MESH = pl.DeviceIdType.MESH
F32 = jnp.float32
BF16 = jnp.bfloat16
LOG2E = math.log2(math.e)

RUN = 256
HD = 128
ROWS = 64


class Slots:
    def __init__(self):
        self.count = 0

    def take(self, n):
        at = self.count
        self.count += n
        return at


SEND = Slots()
RECV = Slots()


def ranges(**sizes):
    return {k: (SEND.take(n), RECV.take(n)) for k, n in sizes.items()}


SEM = ranges(
    xx=4,
    xz=12,
    w1=4,
    w2=12,
    w3=4,
    oy=4,
    oz=4,
    ox=12,
    op=4,
    kv=16,
    kp=16,
    gt=32,
    at=16,
)


def body(
    seq_len,
    x_ref,
    wq_ref,
    wk_ref,
    wv_ref,
    wg_ref,
    fb_ref,
    wo_ref,
    gain_ref,
    out_ref,
    xg,
    wp,
    wg,
    kv,
    gb,
    kbc,
    wo,
    att,
    a_in,
    qt,
    tb,
    acc,
    ms,
    ls,
    zt,
    ssem,
    rsem,
):
    z, y, c, x = (lax.axis_index(n) for n in ("z", "y", "c", "x"))

    def rem4(v):
        return lax.rem(v + 4, 4)

    xr, xl, xo = rem4(x + 1), rem4(x - 1), rem4(x + 2)
    yr, yl, yo = rem4(y + 1), rem4(y - 1), rem4(y + 2)
    zr, zl, zo = rem4(z + 1), rem4(z - 1), rem4(z + 2)
    other = 1 - c

    def copy(src, dst, kind, k, **to):
        s, r = SEM[kind]
        device = {"z": z, "y": y, "c": c, "x": x}
        device.update(to)
        return pltpu.make_async_remote_copy(
            src_ref=src,
            dst_ref=dst,
            send_sem=ssem.at[s + k],
            recv_sem=rsem.at[r + k],
            device_id=device,
            device_id_type=MESH,
        )

    def send(ref, kind, k, **to):
        copy(ref, ref, kind, k, **to).start()

    def got(ref, kind, k):
        copy(ref, ref, kind, k, c=other).wait_recv()

    def sent(ref, kind, k):
        copy(ref, ref, kind, k, c=other).wait_send()

    barrier = pltpu.get_barrier_semaphore()
    peers = []
    for dz in range(4):
        for dx in range(4):
            if dz or dx:
                peers.append(dict(z=rem4(z + dz), x=rem4(x + dx)))
    for dy in range(4):
        for dc in range(2):
            if dy or dc:
                peers.append(dict(y=rem4(y + dy), c=lax.rem(c + dc, 2)))
    for to in peers:
        device = {"z": z, "y": y, "c": c, "x": x}
        device.update(to)
        pl.semaphore_signal(barrier, inc=1, device_id=device, device_id_type=MESH)

    gate = wg_ref[...].astype(F32)
    for h in range(4):
        cols = slice(HD * h, HD * (h + 1))
        wp[h, :, 0:HD] = wq_ref[:, cols]
        wp[h, :, HD : 2 * HD] = wk_ref[:, cols]
        wp[h, :, 2 * HD : 3 * HD] = wv_ref[:, cols]
        wp[h, :, 3 * HD : 4 * HD] = jnp.broadcast_to(gate[:, h : h + 1], (32, HD)).astype(BF16)
    wg[z, y, c] = wp[z]
    xg[z, x] = x_ref[...]
    wo[x, z, y, c] = wo_ref[...]
    pl.semaphore_wait(barrier, len(peers))

    def w1(dz):
        return copy(wp.at[rem4(z + dz)], wg.at[z, y, c], "w1", dz, z=rem4(z + dz))

    def xpiece(zz, xx):
        return xg.at[zz, xx]

    def send_xz(k, xx):
        send(xpiece(z, xx), "xz", k, z=zr)
        send(xpiece(z, xx), "xz", 4 + k, z=zl)

    def wpiece(dz, yy):
        return wg.at[rem4(z - dz), yy, c]

    def send_w2(dz):
        send(wpiece(dz, y), "w2", dz, y=yr)
        send(wpiece(dz, y), "w2", 4 + dz, y=yl)

    for dz in (1, 3, 2):
        w1(dz).start()
    send(xpiece(z, x), "xx", 0, x=xr)
    send(xpiece(z, x), "xx", 1, x=xl)
    send_w2(0)
    send_xz(0, x)
    send(wo.at[x, z, y, c], "oy", 0, y=yr)
    send(wo.at[x, z, y, c], "oy", 1, y=yl)
    for dz in (1, 3, 2):
        got(wpiece(dz, y), "w1", dz)
        send_w2(dz)
    send(wg.at[:, y, c], "w3", 0, c=other)
    half = ROWS // 2
    got(xpiece(z, xl), "xx", 0)
    send(xg.at[z, xl, 0:half], "xx", 2, x=xr)
    send_xz(1, xl)
    got(xpiece(z, xr), "xx", 1)
    send(xg.at[z, xr, half:ROWS], "xx", 3, x=xl)
    send_xz(2, xr)
    for dz in (0, 3):
        got(wpiece(dz, yl), "w2", dz)
        send(wpiece(dz, yl), "w2", 8 + dz, y=yr)
    for dz in (1, 2):
        got(wpiece(dz, yr), "w2", 4 + dz)
        send(wpiece(dz, yr), "w2", 8 + dz, y=yl)
    for dz in (1, 2):
        got(wpiece(dz, yl), "w2", dz)
    send(wg.at[:, yl, c], "w3", 1, c=other)
    for dz in (0, 3):
        got(wpiece(dz, yr), "w2", 4 + dz)
    send(wg.at[:, yr, c], "w3", 2, c=other)
    got(xg.at[z, xo, 0:half], "xx", 2)
    got(xg.at[z, xo, half:ROWS], "xx", 3)
    send_xz(3, xo)
    got(wo.at[x, z, yl, c], "oy", 0)
    send(wo.at[x, z, yl, c, 0:16], "oy", 2, y=yr)
    got(wo.at[x, z, yr, c], "oy", 1)
    send(wo.at[x, z, yr, c, 16:32], "oy", 3, y=yl)
    for dz in (0, 3, 1, 2):
        got(wpiece(dz, yo), "w2", 8 + dz)
    send(wg.at[:, yo, c], "w3", 3, c=other)
    got(wo.at[x, z, yo, c, 0:16], "oy", 2)
    got(wo.at[x, z, yo, c, 16:32], "oy", 3)

    def oslab(xx, dz):
        return wo.at[xx, rem4(z - dz), :, c]

    def send_ox(dz):
        send(oslab(x, dz), "ox", dz, x=xr)
        send(oslab(x, dz), "ox", 4 + dz, x=xl)

    def forward_ox(dz):
        got(oslab(xl, dz), "ox", dz)
        got(oslab(xr, dz), "ox", 4 + dz)
        if dz in (0, 3):
            send(oslab(xl, dz), "ox", 8 + dz, x=xr)
        else:
            send(oslab(xr, dz), "ox", 8 + dz, x=xl)

    send(wo.at[x, z, :, c], "oz", 0, z=zr)
    send(wo.at[x, z, :, c], "oz", 1, z=zl)
    send_ox(0)
    got(wg.at[:, y, other], "w3", 0)
    got(wg.at[:, yl, other], "w3", 1)
    got(wg.at[:, yr, other], "w3", 2)
    got(wg.at[:, yo, other], "w3", 3)

    def level(i):
        first = jnp.where(i == 0, z, 0)
        second = jnp.where(i == 1, jnp.where(z == 0, 1, jnp.where(z == 2, 1, 0)), 0)
        third = jnp.where(i == 2, jnp.where(z == 0, 2, jnp.where(z == 1, 2, jnp.where(z == 2, 0, 1))), 0)
        last = jnp.where(i == 3, jnp.where(z == 3, 2, 3), 0)
        return first + second + third + last

    row = lax.broadcasted_iota(jnp.int32, (RUN, RUN), 0)
    col = lax.broadcasted_iota(jnp.int32, (RUN, RUN), 1)
    tri = jnp.where(row >= col, 1.0, 0.0).astype(BF16)
    offset = fb_ref[z]
    kappa = HD ** (-0.5) * LOG2E

    def gate_peers():
        k = 0
        for dy in range(4):
            for dc in range(2):
                if dy or dc:
                    yield k, rem4(y + dy), lax.rem(c + dc, 2), rem4(y - dy), lax.rem(c + dc, 2)
                k += 1

    def project(i):
        zb = level(i)
        rows = xg[zb].reshape(RUN, 1024)
        weights = wg[...].reshape(1024, 4 * HD)
        out = jnp.dot(rows, weights, preferred_element_type=F32)
        kv[zb, y, c, 0:RUN] = out[:, HD : 2 * HD].astype(BF16)
        vt = out[:, 2 * HD : 3 * HD].T.astype(BF16)
        kv[zb, y, c, RUN : RUN + HD] = vt[:, 0:HD]
        kv[zb, y, c, RUN + HD : RUN + 2 * HD] = vt[:, HD : 2 * HD]
        qt[zb] = out[:, 0:HD].T.astype(BF16)
        raw = out[:, 3 * HD : 4 * HD] + offset + math.log(seq_len)
        lg = jnp.minimum(raw, 0.0) - jnp.log1p(jnp.exp(-jnp.abs(raw)))
        hi = lg.astype(BF16)
        rest = lg - hi.astype(F32)
        mid = rest.astype(BF16)
        low = (rest - mid.astype(F32)).astype(BF16)
        sums = (
            jnp.dot(tri, hi, preferred_element_type=F32)
            + jnp.dot(tri, mid, preferred_element_type=F32)
            + jnp.dot(tri, low, preferred_element_type=F32)
        )
        gb[zb, y, c] = sums.T[0:8]
        for k, ty, tc, _, _ in gate_peers():
            send(gb.at[zb, y, c], "gt", i * 8 + k, y=ty, c=tc)
        send(kv.at[zb, y, c], "kv", i * 4, y=yr)
        send(kv.at[zb, y, c], "kv", i * 4 + 1, y=yl)
        send(kv.at[zb, y, c], "kp", i * 4, c=other)

    def relay(i):
        zb = level(i)
        got(kv.at[zb, yl, c], "kv", i * 4)
        send(kv.at[zb, yl, c, 0:RUN], "kv", i * 4 + 2, y=yr)
        send(kv.at[zb, yl, c], "kp", i * 4 + 1, c=other)
        got(kv.at[zb, yr, c], "kv", i * 4 + 1)
        send(kv.at[zb, yr, c, RUN : 2 * RUN], "kv", i * 4 + 3, y=yl)
        send(kv.at[zb, yr, c], "kp", i * 4 + 2, c=other)

    def gather_level(i):
        zb = level(i)
        got(kv.at[zb, yo, c, 0:RUN], "kv", i * 4 + 2)
        got(kv.at[zb, yo, c, RUN : 2 * RUN], "kv", i * 4 + 3)
        send(kv.at[zb, yo, c], "kp", i * 4 + 3, c=other)
        for k, _, _, sy, sc in gate_peers():
            got(gb.at[zb, sy, sc], "gt", i * 8 + k)
        base = jnp.zeros((8, RUN), F32)
        for yy in range(4):
            for cc in range(2):
                g = gb[zb, yy, cc]
                bias = (g + base) * (-LOG2E)
                kbc[zb, (2 * yy + cc) * RUN : (2 * yy + cc + 1) * RUN] = jnp.concatenate([bias] * 16, axis=0).T
                base = base + jnp.broadcast_to(g[:, RUN - 1 : RUN], (8, RUN))
        zt[zb] = base
        got(kv.at[zb, y, other], "kp", i * 4)
        got(kv.at[zb, yl, other], "kp", i * 4 + 1)
        got(kv.at[zb, yr, other], "kp", i * 4 + 2)
        got(kv.at[zb, yo, other], "kp", i * 4 + 3)

    chunk = 2 * RUN
    ahead = lax.broadcasted_iota(jnp.int32, (chunk, RUN), 0) - lax.broadcasted_iota(jnp.int32, (chunk, RUN), 1)

    def attend(i):
        def one(k, carry):
            late = k == 4
            za = jnp.where(late, level(3), k)
            zb = jnp.where(late, level(0), level(i))
            fits = jnp.where(late, i == 1, jnp.logical_or(i != 0, za != level(3)))

            @pl.when(jnp.logical_and(fits, za >= zb))
            def _():
                pair(za, zb)

            return carry

        def pair(za, zb):
            limit = jnp.where(za == zb, (2 * y + c) * RUN, 4 * chunk)
            top = jnp.full((1, RUN), -1e30, F32)
            for yy in range(4):
                keys = jnp.concatenate([kv[zb, yy, 0, 0:RUN], kv[zb, yy, 1, 0:RUN]], axis=0)
                s = jnp.dot(keys, qt[za], preferred_element_type=F32)
                b = kbc[zb, yy * chunk : (yy + 1) * chunk]
                t = s * kappa + jnp.concatenate([b, b], axis=1)
                t = jnp.where(ahead <= limit - yy * chunk, t, -1e30)
                tb[yy * chunk : (yy + 1) * chunk] = t
                top = jnp.maximum(top, jnp.max(t, axis=0, keepdims=True))
            total = jnp.zeros((1, RUN), F32)
            out = jnp.zeros((HD, RUN), F32)
            for yy in range(4):
                p = jnp.exp2(tb[yy * chunk : (yy + 1) * chunk] - top)
                total = total + jnp.sum(p, axis=0, keepdims=True)
                vt = jnp.concatenate(
                    [
                        kv[zb, yy, cc, RUN + k * HD : RUN + (k + 1) * HD]
                        for cc in range(2)
                        for k in range(2)
                    ],
                    axis=1,
                )
                out = out + jnp.dot(vt, p.astype(BF16), preferred_element_type=F32)
            acc[za, zb] = out
            ms[za, zb] = jnp.broadcast_to(top, (8, RUN))
            ls[za, zb] = jnp.broadcast_to(total, (8, RUN))

        lax.fori_loop(0, 5, one, 0)

    def step(i, carry):
        @pl.when(i == 1)
        def _():
            for k, xx in ((0, rem4(x)), (1, xl), (2, xr), (3, xo)):
                got(xpiece(zl, xx), "xz", k)
                if k in (0, 3):
                    send(xpiece(zl, xx), "xz", 8 + k, z=zr)
                got(xpiece(zr, xx), "xz", 4 + k)
                if k in (1, 2):
                    send(xpiece(zr, xx), "xz", 8 + k, z=zl)
            got(wo.at[x, zl, :, c], "oz", 0)
            send(wo.at[x, zl, 0:2, c], "oz", 2, z=zr)
            got(wo.at[x, zr, :, c], "oz", 1)
            send(wo.at[x, zr, 2:4, c], "oz", 3, z=zl)
            send_ox(1)
            send_ox(3)
            forward_ox(0)

        @pl.when(i == 2)
        def _():
            for k, xx in ((0, rem4(x)), (3, xo), (1, xl), (2, xr)):
                got(xpiece(zo, xx), "xz", 8 + k)

        @pl.when(i < 4)
        def _():
            project(i)

        @pl.when(i == 3)
        def _():
            got(wo.at[x, zo, 0:2, c], "oz", 2)
            got(wo.at[x, zo, 2:4, c], "oz", 3)
            send_ox(2)
            forward_ox(1)
            forward_ox(3)

        @pl.when(jnp.logical_and(i >= 1, i <= 4))
        def _():
            relay(i - 1)

        @pl.when(i == 4)
        def _():
            forward_ox(2)

        @pl.when(i >= 2)
        def _():
            gather_level(i - 2)
            attend(i - 2)

        return carry

    lax.fori_loop(0, 6, step, 0)

    def join(za, carry):
        shift = []
        base = jnp.zeros((8, RUN), F32)
        for zb in range(4):
            shift.append(base * (-LOG2E))
            base = base + zt[zb]
        top = jnp.full((8, RUN), -3e38, F32)
        for zb in range(4):
            top = jnp.where(za >= zb, jnp.maximum(top, ms[za, zb] + shift[zb]), top)
        total = jnp.zeros((8, RUN), F32)
        out = jnp.zeros((HD, RUN), F32)
        for zb in range(4):
            w = jnp.where(za >= zb, jnp.exp2(ms[za, zb] + shift[zb] - top), 0.0)
            total = total + jnp.where(za >= zb, w * ls[za, zb], 0.0)
            out = out + jnp.where(za >= zb, w[0:1] * acc[za, zb], 0.0)
        out = out / total[0:1]
        att[za] = out.T.astype(BF16).reshape(4, ROWS, HD)
        return carry

    lax.fori_loop(0, 4, join, 0)
    a_in[x, z] = att[z, x]

    def rows_to(dz, dx):
        tz, tx = rem4(z + dz), rem4(x + dx)
        return copy(att.at[tz, tx], a_in.at[x, z], "at", dz * 4 + dx, z=tz, x=tx)

    away = [(dz, dx) for dz in range(4) for dx in range(4) if dz or dx]
    for dz, dx in away:
        rows_to(dz, dx).start()
    for dz in (0, 3, 1, 2):
        part = oslab(xo, dz)
        got(part, "ox", 8 + dz)
    for k, xx in enumerate((x, xl, xr, xo)):
        send(wo.at[xx, :, :, c], "op", k, c=other)
    for k, xx in enumerate((x, xl, xr, xo)):
        got(wo.at[xx, :, :, other], "op", k)
    for dz, dx in away:
        got(a_in.at[rem4(x - dx), rem4(z - dz)], "at", dz * 4 + dx)

    summed = jnp.zeros((ROWS, 1024), F32)
    for xx in range(4):
        left = jnp.concatenate([a_in[xx, zz] for zz in range(4)], axis=1)
        right = wo[xx].reshape(1024, 512)
        summed = summed + lax.dot_general(left, right, (((1,), (1,)), ((), ())), preferred_element_type=F32)
    mean = jnp.mean(summed * summed, axis=-1, keepdims=True)
    out_ref[...] = (summed * lax.rsqrt(mean + 1e-06) * gain_ref[...]).astype(BF16)

    for dz in (1, 3, 2):
        w1(dz).wait_send()
    for k, xx in enumerate((x, x, xl, xr)):
        ref = xpiece(z, xx) if k < 2 else xg.at[z, xx, 0:half]
        sent(ref, "xx", k)
    for k in range(12):
        sent(xpiece(z, x), "xz", k)
        sent(wpiece(0, y), "w2", k)
        sent(oslab(x, 0), "ox", k)
    for k in range(4):
        sent(wg.at[:, y, c], "w3", k)
        sent(wo.at[x, z, y, c] if k < 2 else wo.at[x, z, y, c, 0:16], "oy", k)
        sent(wo.at[x, z, :, c] if k < 2 else wo.at[x, z, 0:2, c], "oz", k)
        sent(wo.at[x, :, :, c], "op", k)

    def drain(i, carry):
        for k in range(4):
            sent(kv.at[z, y, c] if k < 2 else kv.at[z, y, c, 0:RUN], "kv", i * 4 + k)
            sent(kv.at[z, y, c], "kp", i * 4 + k)
        for k in range(1, 8):
            sent(gb.at[z, y, c], "gt", i * 8 + k)
        return carry

    lax.fori_loop(0, 4, drain, 0)
    for dz, dx in away:
        rows_to(dz, dx).wait_send()


def local(tokens, query_weight, key_weight, value_weight, gate_weight, forget_bias, out_weight, out_gain):
    seq_len = tokens.shape[0] * lax.axis_size(SP_TP)
    vmem = pl.BlockSpec(memory_space=pltpu.VMEM)

    def kernel(*refs):
        body(seq_len, *refs)

    return pl.pallas_call(
        kernel,
        out_shape=jax.ShapeDtypeStruct(tokens.shape, BF16),
        in_specs=[vmem] * 5 + [pl.BlockSpec(memory_space=pltpu.SMEM)] + [vmem] * 2,
        out_specs=vmem,
        scratch_shapes=[
            pltpu.VMEM((4, 4, ROWS, 1024), BF16),
            pltpu.VMEM((4, 32, 512), BF16),
            pltpu.VMEM((4, 4, 2, 32, 512), BF16),
            pltpu.VMEM((4, 4, 2, 2 * RUN, HD), BF16),
            pltpu.VMEM((4, 4, 2, 8, RUN), F32),
            pltpu.VMEM((4, 8 * RUN, HD), F32),
            pltpu.VMEM((4, 4, 4, 2, 32, 512), BF16),
            pltpu.VMEM((4, 4, ROWS, HD), BF16),
            pltpu.VMEM((4, 4, ROWS, HD), BF16),
            pltpu.VMEM((4, HD, RUN), BF16),
            pltpu.VMEM((8 * RUN, RUN), F32),
            pltpu.VMEM((4, 4, HD, RUN), F32),
            pltpu.VMEM((4, 4, 8, RUN), F32),
            pltpu.VMEM((4, 4, 8, RUN), F32),
            pltpu.VMEM((4, 8, RUN), F32),
            pltpu.SemaphoreType.DMA((SEND.count,)),
            pltpu.SemaphoreType.DMA((RECV.count,)),
        ],
        compiler_params=pltpu.CompilerParams(
            collective_id=0, has_side_effects=True, vmem_limit_bytes=48 * 1024 * 1024
        ),
    )(
        tokens,
        query_weight,
        key_weight,
        value_weight,
        gate_weight,
        forget_bias,
        out_weight.T,
        out_gain.reshape(1, -1),
    )


def solution(mesh):
    torus = Mesh(mesh.devices.reshape(4, 4, 2, mesh.shape["tp"]), SP_TP)
    in_specs = (
        P(SP_TP, None),
        P(SP, "x"),
        P(SP, "x"),
        P(SP, "x"),
        P(SP, "x"),
        P("x"),
        P("x", SP),
        P(),
    )
    out_specs = P(SP_TP, None)
    return jax.shard_map(local, mesh=torus, in_specs=in_specs, out_specs=out_specs, check_vma=False)
```

```python
import math

import jax
import jax.numpy as jnp
from jax import lax
from jax.experimental import pallas as pl
from jax.experimental.pallas import tpu as pltpu
from jax.sharding import Mesh
from jax.sharding import PartitionSpec as P

SP = ("z", "y", "c")
SP_TP = ("z", "y", "c", "x")
MESH = pl.DeviceIdType.MESH
F32 = jnp.float32
BF16 = jnp.bfloat16
LOG2E = math.log2(math.e)

RUN = 256
HD = 128
ROWS = 64


class Slots:
    def __init__(self):
        self.count = 0

    def take(self, n):
        at = self.count
        self.count += n
        return at


SEND = Slots()
RECV = Slots()


def ranges(**sizes):
    return {k: (SEND.take(n), RECV.take(n)) for k, n in sizes.items()}


SEM = ranges(
    xx=4,
    xz=12,
    w1=4,
    w2=12,
    w3=4,
    oy=4,
    oz=4,
    ox=12,
    op=4,
    kv=24,
    kp=16,
    gt=32,
    g1=4,
    g2=8,
    at=16,
)
IN_TOKENS, IN_OUT, IN_GATE, IN_GAIN, IN_OWN, IN_HEADS, IN_COUNT = 0, 1, 2, 3, 4, 7, 19


def body(
    seq_len,
    x_ref,
    wq_ref,
    wk_ref,
    wv_ref,
    wg_ref,
    fb_ref,
    wo_ref,
    gain_ref,
    out_ref,
    xg,
    wp,
    wg,
    kv,
    gb,
    kbc,
    wo,
    att,
    a_in,
    qt,
    tb,
    acc,
    ms,
    ls,
    zt,
    gate_in,
    gain_in,
    grow,
    gwb,
    ssem,
    rsem,
    isem,
):
    z, y, c, x = (lax.axis_index(n) for n in ("z", "y", "c", "x"))

    def rem4(v):
        return lax.rem(v + 4, 4)

    xr, xl, xo = rem4(x + 1), rem4(x - 1), rem4(x + 2)
    yr, yl, yo = rem4(y + 1), rem4(y - 1), rem4(y + 2)
    zr, zl, zo = rem4(z + 1), rem4(z - 1), rem4(z + 2)
    other = 1 - c

    def copy(src, dst, kind, k, **to):
        s, r = SEM[kind]
        device = {"z": z, "y": y, "c": c, "x": x}
        device.update(to)
        return pltpu.make_async_remote_copy(
            src_ref=src,
            dst_ref=dst,
            send_sem=ssem.at[s + k],
            recv_sem=rsem.at[r + k],
            device_id=device,
            device_id_type=MESH,
        )

    def send(ref, kind, k, **to):
        copy(ref, ref, kind, k, **to).start()

    def got(ref, kind, k):
        copy(ref, ref, kind, k, c=other).wait_recv()

    def sent(ref, kind, k):
        copy(ref, ref, kind, k, c=other).wait_send()

    ins = [
        pltpu.make_async_copy(x_ref, xg.at[z, x], isem.at[IN_TOKENS]),
        pltpu.make_async_copy(wg_ref, gate_in, isem.at[IN_GATE]),
        pltpu.make_async_copy(wo_ref, wo.at[x, z, y, c], isem.at[IN_OUT]),
        pltpu.make_async_copy(gain_ref, gain_in, isem.at[IN_GAIN]),
    ]
    own = pl.ds(pl.multiple_of(z * HD, HD), HD)
    for j, ref in enumerate((wq_ref, wk_ref, wv_ref)):
        to = slice(HD * j, HD * (j + 1))
        ins.append(pltpu.make_async_copy(ref.at[:, own], wg.at[z, y, c, :, to], isem.at[IN_OWN + j]))
        for h in range(4):
            cols = slice(HD * h, HD * (h + 1))
            ins.append(
                pltpu.make_async_copy(ref.at[:, cols], wp.at[h, :, to], isem.at[IN_HEADS + 4 * j + h])
            )
    for one in ins:
        one.start()

    barrier = pltpu.get_barrier_semaphore()
    peers = []
    for dz in range(4):
        for dx in range(4):
            if dz or dx:
                peers.append(dict(z=rem4(z + dz), x=rem4(x + dx)))
    for dy in range(4):
        for dc in range(2):
            if dy or dc:
                peers.append(dict(y=rem4(y + dy), c=lax.rem(c + dc, 2)))
    for to in peers:
        device = {"z": z, "y": y, "c": c, "x": x}
        device.update(to)
        pl.semaphore_signal(barrier, inc=1, device_id=device, device_id_type=MESH)

    for one in ins:
        one.wait()
    gate = gate_in[...].astype(F32)
    grow[z, y, c] = jnp.concatenate([gate[h : h + 1] for h in range(4)], axis=1)
    pl.semaphore_wait(barrier, len(peers))

    def gate_peers():
        k = 0
        for dy in range(4):
            for dc in range(2):
                if dy or dc:
                    yield k, rem4(y + dy), lax.rem(c + dc, 2), rem4(y - dy), lax.rem(c + dc, 2)
                k += 1

    def w1(dz):
        return copy(wp.at[rem4(z + dz)], wg.at[z, y, c], "w1", dz, z=rem4(z + dz))

    def xpiece(zz, xx):
        return xg.at[zz, xx]

    def send_xz(k, xx):
        send(xpiece(z, xx), "xz", k, z=zr)
        send(xpiece(z, xx), "xz", 4 + k, z=zl)

    def wpiece(dz, yy):
        return wg.at[rem4(z - dz), yy, c]

    def send_w2(dz):
        send(wpiece(dz, y), "w2", dz, y=yr)
        send(wpiece(dz, y), "w2", 4 + dz, y=yl)

    for dz in (1, 3, 2):
        w1(dz).start()
    send(xpiece(z, x), "xx", 0, x=xr)
    send(xpiece(z, x), "xx", 1, x=xl)
    send_w2(0)
    send_xz(0, x)
    for dz in (1, 3, 2):
        send(grow.at[z, y, c], "g1", dz, z=rem4(z + dz))
    send(wo.at[x, z, y, c], "oy", 0, y=yr)
    send(wo.at[x, z, y, c], "oy", 1, y=yl)
    for dz in (1, 3, 2):
        got(wpiece(dz, y), "w1", dz)
        send_w2(dz)
    send(wg.at[:, y, c], "w3", 0, c=other)
    half = ROWS // 2
    got(xpiece(z, xl), "xx", 0)
    send(xg.at[z, xl, 0:half], "xx", 2, x=xr)
    send_xz(1, xl)
    got(xpiece(z, xr), "xx", 1)
    send(xg.at[z, xr, half:ROWS], "xx", 3, x=xl)
    send_xz(2, xr)
    for dz in (0, 1, 3, 2):
        if dz in (0, 2):
            got(wpiece(dz, yl), "w2", dz)
            send(wpiece(dz, yl), "w2", 8 + dz, y=yr)
        else:
            got(wpiece(dz, yr), "w2", 4 + dz)
            send(wpiece(dz, yr), "w2", 8 + dz, y=yl)
    for dz in (1, 3):
        got(wpiece(dz, yl), "w2", dz)
    send(wg.at[:, yl, c], "w3", 1, c=other)
    for dz in (0, 2):
        got(wpiece(dz, yr), "w2", 4 + dz)
    send(wg.at[:, yr, c], "w3", 2, c=other)
    got(xg.at[z, xo, 0:half], "xx", 2)
    got(xg.at[z, xo, half:ROWS], "xx", 3)
    send_xz(3, xo)
    for dz in (1, 3, 2):
        got(grow.at[rem4(z - dz), y, c], "g1", dz)
    for k, ty, tc, _, _ in gate_peers():
        send(grow.at[:, y, c], "g2", k, y=ty, c=tc)
    got(wo.at[x, z, yl, c], "oy", 0)
    send(wo.at[x, z, yl, c, 0:16], "oy", 2, y=yr)
    got(wo.at[x, z, yr, c], "oy", 1)
    send(wo.at[x, z, yr, c, 16:32], "oy", 3, y=yl)
    for dz in (0, 1, 3, 2):
        got(wpiece(dz, yo), "w2", 8 + dz)
    send(wg.at[:, yo, c], "w3", 3, c=other)
    got(wo.at[x, z, yo, c, 0:16], "oy", 2)
    got(wo.at[x, z, yo, c, 16:32], "oy", 3)

    def oslab(xx, dz):
        return wo.at[xx, rem4(z - dz), :, c]

    def send_ox(dz):
        send(oslab(x, dz), "ox", dz, x=xr)
        send(oslab(x, dz), "ox", 4 + dz, x=xl)

    def forward_ox(dz):
        got(oslab(xl, dz), "ox", dz)
        got(oslab(xr, dz), "ox", 4 + dz)
        if dz in (0, 3):
            send(oslab(xl, dz), "ox", 8 + dz, x=xr)
        else:
            send(oslab(xr, dz), "ox", 8 + dz, x=xl)

    send(wo.at[x, z, :, c], "oz", 0, z=zr)
    send(wo.at[x, z, :, c], "oz", 1, z=zl)
    send_ox(0)
    got(wg.at[:, y, other], "w3", 0)
    got(wg.at[:, yl, other], "w3", 1)
    got(wg.at[:, yr, other], "w3", 2)
    got(wg.at[:, yo, other], "w3", 3)

    def level(i):
        first = jnp.where(i == 0, z, 0)
        second = jnp.where(i == 1, jnp.where(z == 0, 1, jnp.where(z == 2, 1, 0)), 0)
        third = jnp.where(i == 2, jnp.where(z == 0, 2, jnp.where(z == 1, 2, jnp.where(z == 2, 0, 1))), 0)
        last = jnp.where(i == 3, jnp.where(z == 3, 2, 3), 0)
        return first + second + third + last

    row = lax.broadcasted_iota(jnp.int32, (RUN, RUN), 0)
    col = lax.broadcasted_iota(jnp.int32, (RUN, RUN), 1)
    tri = jnp.where(row <= col, 1.0, 0.0).astype(BF16)
    offset = fb_ref[z]
    kappa = HD ** (-0.5) * LOG2E

    def across(a, b):
        return lax.dot_general(a, b, (((1,), (1,)), ((), ())), preferred_element_type=F32)

    place = lax.broadcasted_iota(jnp.int32, (16, RUN), 0)

    def parts(rows):
        hi = rows.astype(BF16).astype(F32)
        mid = (rows - hi).astype(BF16).astype(F32)
        low = rows - hi - mid
        zero = jnp.zeros_like(rows)
        picked = jnp.where(place == 0, hi, jnp.where(place == 1, mid, jnp.where(place == 2, low, zero)))
        return picked.astype(BF16)

    def gate_row():
        for k, _, _, sy, sc in gate_peers():
            got(grow.at[:, sy, sc], "g2", k)
        table = grow[...].reshape(32, HD).astype(BF16)
        deep = lax.broadcasted_iota(jnp.int32, (1024, 32), 0)
        pick = jnp.where(deep // 32 == lax.broadcasted_iota(jnp.int32, (1024, 32), 1), 1.0, 0.0)
        found = jnp.dot(pick.astype(BF16), table, preferred_element_type=F32)
        deep = lax.broadcasted_iota(jnp.int32, (1024, HD), 0)
        lane = lax.broadcasted_iota(jnp.int32, (1024, HD), 1)
        found = jnp.where(lane == 32 * z + deep % 32, found, 0.0).astype(BF16)
        gwb[...] = across(jnp.ones((16, HD), BF16), found).astype(BF16)

    keys, vals = slice(0, RUN), slice(RUN, 2 * RUN)

    def project(i):
        zb = level(i)
        rows = xg[zb].reshape(RUN, 1024)
        weights = wg[...].reshape(1024, 3 * HD)
        out = jnp.dot(rows, weights, preferred_element_type=F32)
        kv[zb, y, c, keys] = out[:, HD : 2 * HD].astype(BF16)
        vt = out[:, 2 * HD : 3 * HD].T.astype(BF16)
        kv[zb, y, c, RUN : RUN + HD] = vt[:, 0:HD]
        kv[zb, y, c, RUN + HD : RUN + 2 * HD] = vt[:, HD : 2 * HD]
        send(kv.at[zb, y, c, keys], "kv", i * 6, y=yr)
        send(kv.at[zb, y, c, vals], "kv", i * 6 + 1, y=yl)
        send(kv.at[zb, y, c, vals], "kv", i * 6 + 2, y=yr)
        send(kv.at[zb, y, c, keys], "kv", i * 6 + 3, y=yl)
        send(kv.at[zb, y, c], "kp", i * 4, c=other)
        q = (out[:, 0:HD].astype(BF16).astype(F32) * kappa).T
        qt[zb, 0:HD] = q.astype(BF16)
        qt[zb, HD : 2 * HD] = (q - q.astype(BF16).astype(F32)).astype(BF16)

        @pl.when(i == 0)
        def _():
            gate_row()

        raw = across(gwb[...], rows) + offset + math.log(seq_len)
        lg = jnp.minimum(raw, 0.0) - jnp.log1p(jnp.exp(-jnp.abs(raw)))
        sums = jnp.dot(parts(lg), tri, preferred_element_type=F32)
        gb[zb, y, c] = jnp.sum(sums, axis=0, keepdims=True)
        for k, ty, tc, _, _ in gate_peers():
            send(gb.at[zb, y, c], "gt", i * 8 + k, y=ty, c=tc)

    def relay(i):
        zb = level(i)
        got(kv.at[zb, yl, c, keys], "kv", i * 6)
        send(kv.at[zb, yl, c, keys], "kv", i * 6 + 4, y=yr)
        got(kv.at[zb, yr, c, vals], "kv", i * 6 + 1)
        send(kv.at[zb, yr, c, vals], "kv", i * 6 + 5, y=yl)
        got(kv.at[zb, yl, c, vals], "kv", i * 6 + 2)
        send(kv.at[zb, yl, c], "kp", i * 4 + 1, c=other)
        got(kv.at[zb, yr, c, keys], "kv", i * 6 + 3)
        send(kv.at[zb, yr, c], "kp", i * 4 + 2, c=other)

    def gather_level(i):
        zb = level(i)
        got(kv.at[zb, yo, c, keys], "kv", i * 6 + 4)
        got(kv.at[zb, yo, c, vals], "kv", i * 6 + 5)
        send(kv.at[zb, yo, c], "kp", i * 4 + 3, c=other)
        for k, _, _, sy, sc in gate_peers():
            got(gb.at[zb, sy, sc], "gt", i * 8 + k)
        base = jnp.zeros((16, RUN), F32)
        bias = []
        for yy in range(4):
            for cc in range(2):
                g = jnp.broadcast_to(gb[zb, yy, cc], (16, RUN))
                bias.append(parts((g + base) * (-LOG2E)))
                base = base + jnp.broadcast_to(g[:, RUN - 1 : RUN], (16, RUN))
        kbc[zb] = lax.dot_general(
            jnp.concatenate(bias, axis=1),
            jnp.ones((16, HD), BF16),
            (((0,), (0,)), ((), ())),
            preferred_element_type=F32,
        )
        zt[zb] = base[0:8]
        got(kv.at[zb, y, other], "kp", i * 4)
        got(kv.at[zb, yl, other], "kp", i * 4 + 1)
        got(kv.at[zb, yr, other], "kp", i * 4 + 2)
        got(kv.at[zb, yo, other], "kp", i * 4 + 3)

    chunk = 2 * RUN
    ahead = lax.broadcasted_iota(jnp.int32, (chunk, RUN), 0) - lax.broadcasted_iota(jnp.int32, (chunk, RUN), 1)

    def attend(i):
        def one(k, carry):
            late = k == 4
            za = jnp.where(late, level(3), k)
            zb = jnp.where(late, level(0), level(i))
            fits = jnp.where(late, i == 1, jnp.logical_or(i != 0, za != level(3)))

            @pl.when(jnp.logical_and(fits, za > zb))
            def _():
                pair(za, zb)

            @pl.when(jnp.logical_and(fits, za == zb))
            def _():
                diagonal(zb)

            return carry

        def logits(za, zb, yy):
            k = jnp.concatenate([kv[zb, yy, 0, 0:RUN], kv[zb, yy, 1, 0:RUN]], axis=0)
            t = jnp.dot(jnp.concatenate([k, k], axis=1), qt[za], preferred_element_type=F32)
            b = kbc[zb, pl.ds(yy * chunk, chunk)]
            return t + jnp.concatenate([b, b], axis=1)

        def weighted(zb, yy, p):
            vt = jnp.concatenate(
                [kv[zb, yy, cc, RUN + k * HD : RUN + (k + 1) * HD] for cc in range(2) for k in range(2)],
                axis=1,
            )
            vt = jnp.concatenate([vt, jnp.ones((16, chunk), BF16)], axis=0)
            return jnp.dot(vt, p.astype(BF16), preferred_element_type=F32)

        def keep(za, zb, out, top):
            acc[za, zb] = out[0:HD]
            ms[za, zb] = jnp.broadcast_to(top, (8, RUN))
            ls[za, zb] = out[HD : HD + 8]

        def pair(za, zb):
            top = jnp.full((1, RUN), -1e30, F32)
            for yy in range(4):
                t = logits(za, zb, yy)
                tb[yy * chunk : (yy + 1) * chunk] = t
                top = jnp.maximum(top, jnp.max(t, axis=0, keepdims=True))
            out = jnp.zeros((HD + 16, RUN), F32)
            for yy in range(4):
                out = out + weighted(zb, yy, jnp.exp2(tb[yy * chunk : (yy + 1) * chunk] - top))
            keep(za, zb, out, top)

        def diagonal(zb):
            def first(yy, top):
                t = logits(zb, zb, yy)
                t = jnp.where(ahead <= (2 * y + c) * RUN - yy * chunk, t, -1e30)
                tb[pl.ds(yy * chunk, chunk)] = t
                return jnp.maximum(top, jnp.max(t, axis=0, keepdims=True))

            top = lax.fori_loop(0, y + 1, first, jnp.full((1, RUN), -1e30, F32))

            def second(yy, out):
                return out + weighted(zb, yy, jnp.exp2(tb[pl.ds(yy * chunk, chunk)] - top))

            keep(zb, zb, lax.fori_loop(0, y + 1, second, jnp.zeros((HD + 16, RUN), F32)), top)

        lax.fori_loop(0, 5, one, 0)

    def step(i, carry):
        @pl.when(i == 1)
        def _():
            for k, xx in ((0, rem4(x)), (1, xl), (2, xr), (3, xo)):
                got(xpiece(zl, xx), "xz", k)
                if k in (0, 3):
                    send(xpiece(zl, xx), "xz", 8 + k, z=zr)
                got(xpiece(zr, xx), "xz", 4 + k)
                if k in (1, 2):
                    send(xpiece(zr, xx), "xz", 8 + k, z=zl)
            got(wo.at[x, zl, :, c], "oz", 0)
            send(wo.at[x, zl, 0:2, c], "oz", 2, z=zr)
            got(wo.at[x, zr, :, c], "oz", 1)
            send(wo.at[x, zr, 2:4, c], "oz", 3, z=zl)
            send_ox(1)
            send_ox(3)
            forward_ox(0)

        @pl.when(i == 2)
        def _():
            for k, xx in ((0, rem4(x)), (3, xo), (1, xl), (2, xr)):
                got(xpiece(zo, xx), "xz", 8 + k)

        @pl.when(i < 4)
        def _():
            project(i)

        @pl.when(i == 3)
        def _():
            got(wo.at[x, zo, 0:2, c], "oz", 2)
            got(wo.at[x, zo, 2:4, c], "oz", 3)
            send_ox(2)
            forward_ox(1)
            forward_ox(3)

        @pl.when(jnp.logical_and(i >= 1, i <= 4))
        def _():
            relay(i - 1)

        @pl.when(i == 4)
        def _():
            forward_ox(2)

        @pl.when(i >= 2)
        def _():
            gather_level(i - 2)
            attend(i - 2)

        return carry

    lax.fori_loop(0, 6, step, 0)

    def rows_to(n, tz, dx):
        tx = rem4(x + dx)
        return copy(att.at[tz, tx], a_in.at[x, z], "at", n * 4 + dx, z=tz, x=tx)

    def send_rows(n, tz, dx):
        rows_to(n, tz, dx).start()

    def join(n, carry):
        za = rem4(z + jnp.where(n == 0, 2, jnp.where(n == 1, 1, jnp.where(n == 2, 3, 0))))
        shift = []
        base = jnp.zeros((8, RUN), F32)
        for zb in range(4):
            shift.append(base * (-LOG2E))
            base = base + zt[zb]
        top = jnp.full((8, RUN), -3e38, F32)
        for zb in range(4):
            top = jnp.where(za >= zb, jnp.maximum(top, ms[za, zb] + shift[zb]), top)
        total = jnp.zeros((8, RUN), F32)
        out = jnp.zeros((HD, RUN), F32)
        for zb in range(4):
            w = jnp.where(za >= zb, jnp.exp2(ms[za, zb] + shift[zb] - top), 0.0)
            total = total + jnp.where(za >= zb, w * ls[za, zb], 0.0)
            out = out + jnp.where(za >= zb, w[0:1] * acc[za, zb], 0.0)
        out = out / total[0:1]
        att[za] = out.T.astype(BF16).reshape(4, ROWS, HD)
        for dx in (2, 1, 3, 0):
            tx = rem4(x + dx)
            if dx:
                send_rows(n, za, dx)
            else:

                @pl.when(n != 3)
                def _():
                    send_rows(n, za, 0)

        return carry

    lax.fori_loop(0, 4, join, 0)
    a_in[x, z] = att[z, x]

    away = [(n, dz, dx) for n, dz in enumerate((2, 1, 3, 0)) for dx in range(4) if dz or dx]
    for dz in (0, 3, 1, 2):
        part = oslab(xo, dz)
        got(part, "ox", 8 + dz)
    for k, xx in enumerate((x, xl, xr, xo)):
        send(wo.at[xx, :, :, c], "op", k, c=other)
    for k, xx in enumerate((x, xl, xr, xo)):
        got(wo.at[xx, :, :, other], "op", k)
    for n, dz, dx in away:
        got(a_in.at[rem4(x - dx), rem4(z - dz)], "at", n * 4 + dx)

    summed = jnp.zeros((ROWS, 1024), F32)
    for xx in range(4):
        left = jnp.concatenate([a_in[xx, zz] for zz in range(4)], axis=1)
        right = wo[xx].reshape(1024, 512)
        summed = summed + lax.dot_general(left, right, (((1,), (1,)), ((), ())), preferred_element_type=F32)
    mean = jnp.mean(summed * summed, axis=-1, keepdims=True)
    out_ref[...] = (summed * lax.rsqrt(mean + 1e-06) * gain_in[...]).astype(BF16)

    for dz in (1, 3, 2):
        w1(dz).wait_send()
        sent(grow.at[z, y, c], "g1", dz)
    for k in range(1, 8):
        sent(grow.at[:, y, c], "g2", k)
    for k, xx in enumerate((x, x, xl, xr)):
        ref = xpiece(z, xx) if k < 2 else xg.at[z, xx, 0:half]
        sent(ref, "xx", k)
    for k in range(12):
        sent(xpiece(z, x), "xz", k)
        sent(wpiece(0, y), "w2", k)
        sent(oslab(x, 0), "ox", k)
    for k in range(4):
        sent(wg.at[:, y, c], "w3", k)
        sent(wo.at[x, z, y, c] if k < 2 else wo.at[x, z, y, c, 0:16], "oy", k)
        sent(wo.at[x, z, :, c] if k < 2 else wo.at[x, z, 0:2, c], "oz", k)
        sent(wo.at[x, :, :, c], "op", k)

    def drain(i, carry):
        for k in range(4):
            sent(kv.at[z, y, c], "kp", i * 4 + k)
        for k in range(6):
            sent(kv.at[z, y, c, keys], "kv", i * 6 + k)
        for k in range(1, 8):
            sent(gb.at[z, y, c], "gt", i * 8 + k)
        return carry

    lax.fori_loop(0, 4, drain, 0)
    for n, dz, dx in away:
        rows_to(n, rem4(z + dz), dx).wait_send()


def local(tokens, query_weight, key_weight, value_weight, gate_weight, forget_bias, out_weight, out_gain):
    seq_len = tokens.shape[0] * lax.axis_size(SP_TP)
    vmem = pl.BlockSpec(memory_space=pltpu.VMEM)
    hbm = pl.BlockSpec(memory_space=pltpu.HBM)

    def kernel(*refs):
        body(seq_len, *refs)

    return pl.pallas_call(
        kernel,
        out_shape=jax.ShapeDtypeStruct(tokens.shape, BF16),
        in_specs=[hbm] * 5 + [pl.BlockSpec(memory_space=pltpu.SMEM)] + [hbm] * 2,
        out_specs=vmem,
        scratch_shapes=[
            pltpu.VMEM((4, 4, ROWS, 1024), BF16),
            pltpu.VMEM((4, 32, 3 * HD), BF16),
            pltpu.VMEM((4, 4, 2, 32, 3 * HD), BF16),
            pltpu.VMEM((4, 4, 2, 2 * RUN, HD), BF16),
            pltpu.VMEM((4, 4, 2, 1, RUN), F32),
            pltpu.VMEM((4, 8 * RUN, HD), F32),
            pltpu.VMEM((4, 4, 4, 2, 32, 512), BF16),
            pltpu.VMEM((4, 4, ROWS, HD), BF16),
            pltpu.VMEM((4, 4, ROWS, HD), BF16),
            pltpu.VMEM((4, 2 * HD, RUN), BF16),
            pltpu.VMEM((8 * RUN, RUN), F32),
            pltpu.VMEM((4, 4, HD, RUN), F32),
            pltpu.VMEM((4, 4, 8, RUN), F32),
            pltpu.VMEM((4, 4, 8, RUN), F32),
            pltpu.VMEM((4, 8, RUN), F32),
            pltpu.VMEM((4, 32), BF16),
            pltpu.VMEM((1, 1024), F32),
            pltpu.VMEM((4, 4, 2, 1, HD), F32),
            pltpu.VMEM((16, 1024), BF16),
            pltpu.SemaphoreType.DMA((SEND.count,)),
            pltpu.SemaphoreType.DMA((RECV.count,)),
            pltpu.SemaphoreType.DMA((IN_COUNT,)),
        ],
        compiler_params=pltpu.CompilerParams(
            collective_id=0, has_side_effects=True, vmem_limit_bytes=67043328
        ),
    )(
        tokens,
        query_weight,
        key_weight,
        value_weight,
        gate_weight.T,
        forget_bias,
        out_weight.T,
        out_gain.reshape(1, -1),
    )


def solution(mesh):
    torus = Mesh(mesh.devices.reshape(4, 4, 2, mesh.shape["tp"]), SP_TP)
    in_specs = (
        P(SP_TP, None),
        P(SP, "x"),
        P(SP, "x"),
        P(SP, "x"),
        P(SP, "x"),
        P("x"),
        P("x", SP),
        P(),
    )
    out_specs = P(SP_TP, None)
    return jax.shard_map(local, mesh=torus, in_specs=in_specs, out_specs=out_specs, check_vma=False)
```

```python
import math

import jax
import jax.numpy as jnp
from jax import lax
from jax.experimental import pallas as pl
from jax.experimental.pallas import tpu as pltpu
from jax.sharding import Mesh
from jax.sharding import PartitionSpec as P

SP = ("z", "y", "c")
SP_TP = ("z", "y", "c", "x")
MESH = pl.DeviceIdType.MESH
F32 = jnp.float32
BF16 = jnp.bfloat16
LOG2E = math.log2(math.e)

RUN = 256
HD = 128
ROWS = 64


class Slots:
    def __init__(self):
        self.count = 0

    def take(self, n):
        at = self.count
        self.count += n
        return at


SEND = Slots()
RECV = Slots()


def ranges(**sizes):
    return {k: (SEND.take(n), RECV.take(n)) for k, n in sizes.items()}


SEM = ranges(
    xx=4,
    xz=12,
    w1=4,
    w2=12,
    w3=4,
    oy=4,
    oz=4,
    ox=12,
    op=4,
    kv=24,
    kp=16,
    gt=32,
    g1=4,
    g2=8,
    at=16,
)
IN_TOKENS, IN_OUT, IN_GATE, IN_GAIN, IN_OWN, IN_HEADS, IN_COUNT = 0, 1, 2, 3, 4, 7, 19


def body(
    seq_len,
    x_ref,
    wq_ref,
    wk_ref,
    wv_ref,
    wg_ref,
    fb_ref,
    wo_ref,
    gain_ref,
    out_ref,
    xg,
    wp,
    wg,
    kv,
    gb,
    kbc,
    wo,
    att,
    a_in,
    qt,
    tb,
    acc,
    ms,
    ls,
    zt,
    gate_in,
    gain_in,
    grow,
    gwb,
    ssem,
    rsem,
    isem,
):
    z, y, c, x = (lax.axis_index(n) for n in ("z", "y", "c", "x"))

    def rem4(v):
        return lax.rem(v + 4, 4)

    xr, xl, xo = rem4(x + 1), rem4(x - 1), rem4(x + 2)
    yr, yl, yo = rem4(y + 1), rem4(y - 1), rem4(y + 2)
    zr, zl, zo = rem4(z + 1), rem4(z - 1), rem4(z + 2)
    other = 1 - c

    def copy(src, dst, kind, k, **to):
        s, r = SEM[kind]
        device = {"z": z, "y": y, "c": c, "x": x}
        device.update(to)
        return pltpu.make_async_remote_copy(
            src_ref=src,
            dst_ref=dst,
            send_sem=ssem.at[s + k],
            recv_sem=rsem.at[r + k],
            device_id=device,
            device_id_type=MESH,
        )

    def send(ref, kind, k, **to):
        copy(ref, ref, kind, k, **to).start()

    def got(ref, kind, k):
        copy(ref, ref, kind, k, c=other).wait_recv()

    def sent(ref, kind, k):
        copy(ref, ref, kind, k, c=other).wait_send()

    ins = [
        pltpu.make_async_copy(x_ref, xg.at[z, x], isem.at[IN_TOKENS]),
        pltpu.make_async_copy(wg_ref, gate_in, isem.at[IN_GATE]),
        pltpu.make_async_copy(wo_ref, wo.at[x, z, y, c], isem.at[IN_OUT]),
        pltpu.make_async_copy(gain_ref, gain_in, isem.at[IN_GAIN]),
    ]
    own = pl.ds(pl.multiple_of(z * HD, HD), HD)
    for j, ref in enumerate((wq_ref, wk_ref, wv_ref)):
        to = slice(HD * j, HD * (j + 1))
        ins.append(pltpu.make_async_copy(ref.at[:, own], wg.at[z, y, c, :, to], isem.at[IN_OWN + j]))
        for h in range(4):
            cols = slice(HD * h, HD * (h + 1))
            ins.append(
                pltpu.make_async_copy(ref.at[:, cols], wp.at[h, :, to], isem.at[IN_HEADS + 4 * j + h])
            )
    for one in ins:
        one.start()

    barrier = pltpu.get_barrier_semaphore()
    peers = []
    for dz in range(4):
        for dx in range(4):
            if dz or dx:
                peers.append(dict(z=rem4(z + dz), x=rem4(x + dx)))
    for dy in range(4):
        for dc in range(2):
            if dy or dc:
                peers.append(dict(y=rem4(y + dy), c=lax.rem(c + dc, 2)))
    for to in peers:
        device = {"z": z, "y": y, "c": c, "x": x}
        device.update(to)
        pl.semaphore_signal(barrier, inc=1, device_id=device, device_id_type=MESH)

    for one in ins:
        one.wait()
    gate = gate_in[...].astype(F32)
    grow[z, y, c] = jnp.concatenate([gate[h : h + 1] for h in range(4)], axis=1)
    pl.semaphore_wait(barrier, len(peers))

    def gate_peers():
        k = 0
        for dy in range(4):
            for dc in range(2):
                if dy or dc:
                    yield k, rem4(y + dy), lax.rem(c + dc, 2), rem4(y - dy), lax.rem(c + dc, 2)
                k += 1

    def w1(dz):
        return copy(wp.at[rem4(z + dz)], wg.at[z, y, c], "w1", dz, z=rem4(z + dz))

    def xpiece(zz, xx):
        return xg.at[zz, xx]

    def send_xz(k, xx):
        send(xpiece(z, xx), "xz", k, z=zr)
        send(xpiece(z, xx), "xz", 4 + k, z=zl)

    def wpiece(dz, yy):
        return wg.at[rem4(z - dz), yy, c]

    def send_w2(dz):
        send(wpiece(dz, y), "w2", dz, y=yr)
        send(wpiece(dz, y), "w2", 4 + dz, y=yl)

    for dz in (1, 3, 2):
        w1(dz).start()
    send(xpiece(z, x), "xx", 0, x=xr)
    send(xpiece(z, x), "xx", 1, x=xl)
    send_w2(0)
    send_xz(0, x)
    for dz in (1, 3, 2):
        send(grow.at[z, y, c], "g1", dz, z=rem4(z + dz))
    send(wo.at[x, z, y, c], "oy", 0, y=yr)
    send(wo.at[x, z, y, c], "oy", 1, y=yl)
    for dz in (1, 3, 2):
        got(wpiece(dz, y), "w1", dz)
        send_w2(dz)
    send(wg.at[:, y, c], "w3", 0, c=other)
    half = ROWS // 2
    got(xpiece(z, xl), "xx", 0)
    send(xg.at[z, xl, 0:half], "xx", 2, x=xr)
    send_xz(1, xl)
    got(xpiece(z, xr), "xx", 1)
    send(xg.at[z, xr, half:ROWS], "xx", 3, x=xl)
    send_xz(2, xr)
    for dz in (0, 1, 3, 2):
        if dz in (0, 2):
            got(wpiece(dz, yl), "w2", dz)
            send(wpiece(dz, yl), "w2", 8 + dz, y=yr)
        else:
            got(wpiece(dz, yr), "w2", 4 + dz)
            send(wpiece(dz, yr), "w2", 8 + dz, y=yl)
    for dz in (1, 3):
        got(wpiece(dz, yl), "w2", dz)
    send(wg.at[:, yl, c], "w3", 1, c=other)
    for dz in (0, 2):
        got(wpiece(dz, yr), "w2", 4 + dz)
    send(wg.at[:, yr, c], "w3", 2, c=other)
    got(xg.at[z, xo, 0:half], "xx", 2)
    got(xg.at[z, xo, half:ROWS], "xx", 3)
    send_xz(3, xo)
    for dz in (1, 3, 2):
        got(grow.at[rem4(z - dz), y, c], "g1", dz)
    for k, ty, tc, _, _ in gate_peers():
        send(grow.at[:, y, c], "g2", k, y=ty, c=tc)
    got(wo.at[x, z, yl, c], "oy", 0)
    send(wo.at[x, z, yl, c, 0:16], "oy", 2, y=yr)
    got(wo.at[x, z, yr, c], "oy", 1)
    send(wo.at[x, z, yr, c, 16:32], "oy", 3, y=yl)
    for dz in (0, 1, 3, 2):
        got(wpiece(dz, yo), "w2", 8 + dz)
    send(wg.at[:, yo, c], "w3", 3, c=other)
    got(wo.at[x, z, yo, c, 0:16], "oy", 2)
    got(wo.at[x, z, yo, c, 16:32], "oy", 3)

    def oslab(xx, dz):
        return wo.at[xx, rem4(z - dz), :, c]

    def send_ox(dz):
        send(oslab(x, dz), "ox", dz, x=xr)
        send(oslab(x, dz), "ox", 4 + dz, x=xl)

    def forward_ox(dz):
        got(oslab(xl, dz), "ox", dz)
        got(oslab(xr, dz), "ox", 4 + dz)
        if dz in (0, 3):
            send(oslab(xl, dz), "ox", 8 + dz, x=xr)
        else:
            send(oslab(xr, dz), "ox", 8 + dz, x=xl)

    send(wo.at[x, z, :, c], "oz", 0, z=zr)
    send(wo.at[x, z, :, c], "oz", 1, z=zl)
    send_ox(0)

    def relay_xz(k, xx):
        got(xpiece(zl, xx), "xz", k)
        if k in (0, 3):
            send(xpiece(zl, xx), "xz", 8 + k, z=zr)
        got(xpiece(zr, xx), "xz", 4 + k)
        if k in (1, 2):
            send(xpiece(zr, xx), "xz", 8 + k, z=zl)

    for k, xx in ((0, x), (1, xl), (2, xr)):
        relay_xz(k, xx)
    got(wg.at[:, y, other], "w3", 0)
    got(wg.at[:, yl, other], "w3", 1)
    got(wg.at[:, yr, other], "w3", 2)
    got(wg.at[:, yo, other], "w3", 3)

    def level(i):
        first = jnp.where(i == 0, z, 0)
        second = jnp.where(i == 1, jnp.where(z == 0, 1, jnp.where(z == 2, 1, 0)), 0)
        third = jnp.where(i == 2, jnp.where(z == 0, 2, jnp.where(z == 1, 2, jnp.where(z == 2, 0, 1))), 0)
        last = jnp.where(i == 3, jnp.where(z == 3, 2, 3), 0)
        return first + second + third + last

    row = lax.broadcasted_iota(jnp.int32, (RUN, RUN), 0)
    col = lax.broadcasted_iota(jnp.int32, (RUN, RUN), 1)
    tri = jnp.where(row <= col, 1.0, 0.0).astype(BF16)
    offset = fb_ref[z]
    kappa = HD ** (-0.5) * LOG2E

    def across(a, b):
        return lax.dot_general(a, b, (((1,), (1,)), ((), ())), preferred_element_type=F32)

    place = lax.broadcasted_iota(jnp.int32, (16, RUN), 0)

    def parts(rows):
        hi = rows.astype(BF16).astype(F32)
        mid = (rows - hi).astype(BF16).astype(F32)
        low = rows - hi - mid
        zero = jnp.zeros_like(rows)
        picked = jnp.where(place == 0, hi, jnp.where(place == 1, mid, jnp.where(place == 2, low, zero)))
        return picked.astype(BF16)

    def gate_row():
        for k, _, _, sy, sc in gate_peers():
            got(grow.at[:, sy, sc], "g2", k)
        table = grow[...].reshape(32, HD).astype(BF16)
        deep = lax.broadcasted_iota(jnp.int32, (1024, 32), 0)
        pick = jnp.where(deep // 32 == lax.broadcasted_iota(jnp.int32, (1024, 32), 1), 1.0, 0.0)
        found = jnp.dot(pick.astype(BF16), table, preferred_element_type=F32)
        deep = lax.broadcasted_iota(jnp.int32, (1024, HD), 0)
        lane = lax.broadcasted_iota(jnp.int32, (1024, HD), 1)
        found = jnp.where(lane == 32 * z + deep % 32, found, 0.0).astype(BF16)
        gwb[...] = across(jnp.ones((16, HD), BF16), found).astype(BF16)

    keys, vals = slice(0, RUN), slice(RUN, 2 * RUN)

    def project(i):
        zb = level(i)
        rows = xg[zb].reshape(RUN, 1024)
        weights = wg[...].reshape(1024, 3 * HD)
        out = jnp.dot(rows, weights, preferred_element_type=F32)
        kv[zb, y, c, keys] = out[:, HD : 2 * HD].astype(BF16)
        vt = out[:, 2 * HD : 3 * HD].T.astype(BF16)
        kv[zb, y, c, RUN : RUN + HD] = vt[:, 0:HD]
        kv[zb, y, c, RUN + HD : RUN + 2 * HD] = vt[:, HD : 2 * HD]
        send(kv.at[zb, y, c, keys], "kv", i * 6, y=yr)
        send(kv.at[zb, y, c, vals], "kv", i * 6 + 1, y=yl)
        send(kv.at[zb, y, c, vals], "kv", i * 6 + 2, y=yr)
        send(kv.at[zb, y, c, keys], "kv", i * 6 + 3, y=yl)
        send(kv.at[zb, y, c], "kp", i * 4, c=other)
        q = (out[:, 0:HD].astype(BF16).astype(F32) * kappa).T
        qt[zb, 0:HD] = q.astype(BF16)
        qt[zb, HD : 2 * HD] = (q - q.astype(BF16).astype(F32)).astype(BF16)

        @pl.when(i == 0)
        def _():
            gate_row()

        raw = across(gwb[...], rows) + offset + math.log(seq_len)
        lg = jnp.minimum(raw, 0.0) - jnp.log1p(jnp.exp(-jnp.abs(raw)))
        sums = jnp.dot(parts(lg), tri, preferred_element_type=F32)
        gb[zb, y, c] = jnp.sum(sums, axis=0, keepdims=True)
        for k, ty, tc, _, _ in gate_peers():
            send(gb.at[zb, y, c], "gt", i * 8 + k, y=ty, c=tc)

    def relay(i):
        zb = level(i)
        got(kv.at[zb, yl, c, keys], "kv", i * 6)
        send(kv.at[zb, yl, c, keys], "kv", i * 6 + 4, y=yr)
        got(kv.at[zb, yr, c, vals], "kv", i * 6 + 1)
        send(kv.at[zb, yr, c, vals], "kv", i * 6 + 5, y=yl)
        got(kv.at[zb, yl, c, vals], "kv", i * 6 + 2)
        send(kv.at[zb, yl, c], "kp", i * 4 + 1, c=other)
        got(kv.at[zb, yr, c, keys], "kv", i * 6 + 3)
        send(kv.at[zb, yr, c], "kp", i * 4 + 2, c=other)

    def gather_level(i):
        zb = level(i)
        got(kv.at[zb, yo, c, keys], "kv", i * 6 + 4)
        got(kv.at[zb, yo, c, vals], "kv", i * 6 + 5)
        send(kv.at[zb, yo, c], "kp", i * 4 + 3, c=other)
        for k, _, _, sy, sc in gate_peers():
            got(gb.at[zb, sy, sc], "gt", i * 8 + k)
        base = jnp.zeros((16, RUN), F32)
        bias = []
        for yy in range(4):
            for cc in range(2):
                g = jnp.broadcast_to(gb[zb, yy, cc], (16, RUN))
                bias.append(parts((g + base) * (-LOG2E)))
                base = base + jnp.broadcast_to(g[:, RUN - 1 : RUN], (16, RUN))
        kbc[zb] = lax.dot_general(
            jnp.concatenate(bias, axis=1),
            jnp.ones((16, HD), BF16),
            (((0,), (0,)), ((), ())),
            preferred_element_type=F32,
        )
        zt[zb] = base[0:8]
        got(kv.at[zb, y, other], "kp", i * 4)
        got(kv.at[zb, yl, other], "kp", i * 4 + 1)
        got(kv.at[zb, yr, other], "kp", i * 4 + 2)
        got(kv.at[zb, yo, other], "kp", i * 4 + 3)

    chunk = 2 * RUN
    ahead = lax.broadcasted_iota(jnp.int32, (chunk, RUN), 0) - lax.broadcasted_iota(jnp.int32, (chunk, RUN), 1)

    def attend(i):
        def one(k, carry):
            late = k == 4
            za = jnp.where(late, level(3), k)
            zb = jnp.where(late, level(0), level(i))
            fits = jnp.where(late, i == 1, jnp.logical_or(i != 0, za != level(3)))

            @pl.when(jnp.logical_and(fits, za > zb))
            def _():
                pair(za, zb)

            @pl.when(jnp.logical_and(fits, za == zb))
            def _():
                diagonal(zb)

            return carry

        def logits(za, zb, yy):
            k = jnp.concatenate([kv[zb, yy, 0, 0:RUN], kv[zb, yy, 1, 0:RUN]], axis=0)
            t = jnp.dot(jnp.concatenate([k, k], axis=1), qt[za], preferred_element_type=F32)
            b = kbc[zb, pl.ds(yy * chunk, chunk)]
            return t + jnp.concatenate([b, b], axis=1)

        def weighted(zb, yy, p):
            vt = jnp.concatenate(
                [kv[zb, yy, cc, RUN + k * HD : RUN + (k + 1) * HD] for cc in range(2) for k in range(2)],
                axis=1,
            )
            vt = jnp.concatenate([vt, jnp.ones((16, chunk), BF16)], axis=0)
            return jnp.dot(vt, p.astype(BF16), preferred_element_type=F32)

        def keep(za, zb, out, top):
            acc[za, zb] = out[0:HD]
            ms[za, zb] = jnp.broadcast_to(top, (8, RUN))
            ls[za, zb] = out[HD : HD + 8]

        def pair(za, zb):
            top = jnp.full((1, RUN), -1e30, F32)
            for yy in range(4):
                t = logits(za, zb, yy)
                tb[yy * chunk : (yy + 1) * chunk] = t
                top = jnp.maximum(top, jnp.max(t, axis=0, keepdims=True))
            out = jnp.zeros((HD + 16, RUN), F32)
            for yy in range(4):
                out = out + weighted(zb, yy, jnp.exp2(tb[yy * chunk : (yy + 1) * chunk] - top))
            keep(za, zb, out, top)

        def diagonal(zb):
            def first(yy, top):
                t = logits(zb, zb, yy)
                t = jnp.where(ahead <= (2 * y + c) * RUN - yy * chunk, t, -1e30)
                tb[pl.ds(yy * chunk, chunk)] = t
                return jnp.maximum(top, jnp.max(t, axis=0, keepdims=True))

            top = lax.fori_loop(0, y + 1, first, jnp.full((1, RUN), -1e30, F32))

            def second(yy, out):
                return out + weighted(zb, yy, jnp.exp2(tb[pl.ds(yy * chunk, chunk)] - top))

            keep(zb, zb, lax.fori_loop(0, y + 1, second, jnp.zeros((HD + 16, RUN), F32)), top)

        lax.fori_loop(0, 5, one, 0)

    def step(i, carry):
        @pl.when(i == 1)
        def _():
            relay_xz(3, xo)
            got(wo.at[x, zl, :, c], "oz", 0)
            send(wo.at[x, zl, 0:2, c], "oz", 2, z=zr)
            got(wo.at[x, zr, :, c], "oz", 1)
            send(wo.at[x, zr, 2:4, c], "oz", 3, z=zl)
            send_ox(1)
            send_ox(3)
            forward_ox(0)

        @pl.when(i == 2)
        def _():
            for k, xx in ((0, rem4(x)), (3, xo), (1, xl), (2, xr)):
                got(xpiece(zo, xx), "xz", 8 + k)

        @pl.when(i < 4)
        def _():
            project(i)

        @pl.when(i == 3)
        def _():
            got(wo.at[x, zo, 0:2, c], "oz", 2)
            got(wo.at[x, zo, 2:4, c], "oz", 3)
            send_ox(2)
            forward_ox(1)
            forward_ox(3)

        @pl.when(jnp.logical_and(i >= 1, i <= 4))
        def _():
            relay(i - 1)

        @pl.when(i == 4)
        def _():
            forward_ox(2)

        @pl.when(i >= 2)
        def _():
            gather_level(i - 2)
            attend(i - 2)

        return carry

    lax.fori_loop(0, 6, step, 0)

    def rows_to(n, tz, dx):
        tx = rem4(x + dx)
        return copy(att.at[tz, tx], a_in.at[x, z], "at", n * 4 + dx, z=tz, x=tx)

    def send_rows(n, tz, dx):
        rows_to(n, tz, dx).start()

    def join(n, carry):
        za = rem4(z + jnp.where(n == 0, 2, jnp.where(n == 1, 1, jnp.where(n == 2, 3, 0))))
        shift = []
        base = jnp.zeros((8, RUN), F32)
        for zb in range(4):
            shift.append(base * (-LOG2E))
            base = base + zt[zb]
        top = jnp.full((8, RUN), -3e38, F32)
        for zb in range(4):
            top = jnp.where(za >= zb, jnp.maximum(top, ms[za, zb] + shift[zb]), top)
        total = jnp.zeros((8, RUN), F32)
        out = jnp.zeros((HD, RUN), F32)
        for zb in range(4):
            w = jnp.where(za >= zb, jnp.exp2(ms[za, zb] + shift[zb] - top), 0.0)
            total = total + jnp.where(za >= zb, w * ls[za, zb], 0.0)
            out = out + jnp.where(za >= zb, w[0:1] * acc[za, zb], 0.0)
        out = out / total[0:1]
        att[za] = out.T.astype(BF16).reshape(4, ROWS, HD)
        for dx in (2, 1, 3, 0):
            tx = rem4(x + dx)
            if dx:
                send_rows(n, za, dx)
            else:

                @pl.when(n != 3)
                def _():
                    send_rows(n, za, 0)

        return carry

    lax.fori_loop(0, 4, join, 0)
    a_in[x, z] = att[z, x]

    away = [(n, dz, dx) for n, dz in enumerate((2, 1, 3, 0)) for dx in range(4) if dz or dx]
    for dz in (0, 3, 1, 2):
        part = oslab(xo, dz)
        got(part, "ox", 8 + dz)
    for k, xx in enumerate((x, xl, xr, xo)):
        send(wo.at[xx, :, :, c], "op", k, c=other)
    for k, xx in enumerate((x, xl, xr, xo)):
        got(wo.at[xx, :, :, other], "op", k)
    for n, dz, dx in away:
        got(a_in.at[rem4(x - dx), rem4(z - dz)], "at", n * 4 + dx)

    summed = jnp.zeros((ROWS, 1024), F32)
    for xx in range(4):
        left = jnp.concatenate([a_in[xx, zz] for zz in range(4)], axis=1)
        right = wo[xx].reshape(1024, 512)
        summed = summed + lax.dot_general(left, right, (((1,), (1,)), ((), ())), preferred_element_type=F32)
    mean = jnp.mean(summed * summed, axis=-1, keepdims=True)
    out_ref[...] = (summed * lax.rsqrt(mean + 1e-06) * gain_in[...]).astype(BF16)

    for dz in (1, 3, 2):
        w1(dz).wait_send()
        sent(grow.at[z, y, c], "g1", dz)
    for k in range(1, 8):
        sent(grow.at[:, y, c], "g2", k)
    for k, xx in enumerate((x, x, xl, xr)):
        ref = xpiece(z, xx) if k < 2 else xg.at[z, xx, 0:half]
        sent(ref, "xx", k)
    for k in range(12):
        sent(xpiece(z, x), "xz", k)
        sent(wpiece(0, y), "w2", k)
        sent(oslab(x, 0), "ox", k)
    for k in range(4):
        sent(wg.at[:, y, c], "w3", k)
        sent(wo.at[x, z, y, c] if k < 2 else wo.at[x, z, y, c, 0:16], "oy", k)
        sent(wo.at[x, z, :, c] if k < 2 else wo.at[x, z, 0:2, c], "oz", k)
        sent(wo.at[x, :, :, c], "op", k)

    def drain(i, carry):
        for k in range(4):
            sent(kv.at[z, y, c], "kp", i * 4 + k)
        for k in range(6):
            sent(kv.at[z, y, c, keys], "kv", i * 6 + k)
        for k in range(1, 8):
            sent(gb.at[z, y, c], "gt", i * 8 + k)
        return carry

    lax.fori_loop(0, 4, drain, 0)
    for n, dz, dx in away:
        rows_to(n, rem4(z + dz), dx).wait_send()


def local(tokens, query_weight, key_weight, value_weight, gate_weight, forget_bias, out_weight, out_gain):
    seq_len = tokens.shape[0] * lax.axis_size(SP_TP)
    vmem = pl.BlockSpec(memory_space=pltpu.VMEM)
    hbm = pl.BlockSpec(memory_space=pltpu.HBM)

    def kernel(*refs):
        body(seq_len, *refs)

    return pl.pallas_call(
        kernel,
        out_shape=jax.ShapeDtypeStruct(tokens.shape, BF16),
        in_specs=[hbm] * 5 + [pl.BlockSpec(memory_space=pltpu.SMEM)] + [hbm] * 2,
        out_specs=vmem,
        scratch_shapes=[
            pltpu.VMEM((4, 4, ROWS, 1024), BF16),
            pltpu.VMEM((4, 32, 3 * HD), BF16),
            pltpu.VMEM((4, 4, 2, 32, 3 * HD), BF16),
            pltpu.VMEM((4, 4, 2, 2 * RUN, HD), BF16),
            pltpu.VMEM((4, 4, 2, 1, RUN), F32),
            pltpu.VMEM((4, 8 * RUN, HD), F32),
            pltpu.VMEM((4, 4, 4, 2, 32, 512), BF16),
            pltpu.VMEM((4, 4, ROWS, HD), BF16),
            pltpu.VMEM((4, 4, ROWS, HD), BF16),
            pltpu.VMEM((4, 2 * HD, RUN), BF16),
            pltpu.VMEM((8 * RUN, RUN), F32),
            pltpu.VMEM((4, 4, HD, RUN), F32),
            pltpu.VMEM((4, 4, 8, RUN), F32),
            pltpu.VMEM((4, 4, 8, RUN), F32),
            pltpu.VMEM((4, 8, RUN), F32),
            pltpu.VMEM((4, 32), BF16),
            pltpu.VMEM((1, 1024), F32),
            pltpu.VMEM((4, 4, 2, 1, HD), F32),
            pltpu.VMEM((16, 1024), BF16),
            pltpu.SemaphoreType.DMA((SEND.count,)),
            pltpu.SemaphoreType.DMA((RECV.count,)),
            pltpu.SemaphoreType.DMA((IN_COUNT,)),
        ],
        compiler_params=pltpu.CompilerParams(
            collective_id=0, has_side_effects=True, vmem_limit_bytes=67043328
        ),
    )(
        tokens,
        query_weight,
        key_weight,
        value_weight,
        gate_weight.T,
        forget_bias,
        out_weight.T,
        out_gain.reshape(1, -1),
    )


def solution(mesh):
    torus = Mesh(mesh.devices.reshape(4, 4, 2, mesh.shape["tp"]), SP_TP)
    in_specs = (
        P(SP_TP, None),
        P(SP, "x"),
        P(SP, "x"),
        P(SP, "x"),
        P(SP, "x"),
        P("x"),
        P("x", SP),
        P(),
    )
    out_specs = P(SP_TP, None)
    return jax.shard_map(local, mesh=torus, in_specs=in_specs, out_specs=out_specs, check_vma=False)
```
